32 devices in a mesh: fs: 4 (over y, x), tp: 8 (over z, core).
Axes of the slice: x: 2, y: 2, z: 4, core: 2. Of those that a mesh axis runs over, the one named last changes fastest.
Arguments:
- tokens: bfloat16 [4096, 2048], P(('fs', 'tp')), may hold values from -6 to 6
- up_gate: bfloat16 [4096, 5632], P('fs', 'tp'), may hold values from -8 to 8
- up_val: bfloat16 [4096, 5632], P('fs', 'tp'), may hold values from -6 to 6
- gate_weight: bfloat16 [2048, 5632], P('fs', 'tp'), may hold values from -0.125 to 0.125
- val_weight: bfloat16 [2048, 5632], P('fs', 'tp'), may hold values from -0.125 to 0.125
- gate_taps: bfloat16 [3, 5632], P(None, 'tp'), may hold values from -3 to 3
- val_taps: bfloat16 [3, 5632], P(None, 'tp'), may hold values from -3 to 3
- hidden_grad: bfloat16 [4096, 5632], P('fs', 'tp'), may hold values from -6 to 6
Outputs:
- input_grad: bfloat16 [4096, 2048], P(('fs', 'tp'))
- gate_weight_grad: float32 [2048, 5632], P('fs', 'tp')
- val_weight_grad: float32 [2048, 5632], P('fs', 'tp')
- gate_taps_grad: float32 [3, 5632], P(None, 'tp')
- val_taps_grad: float32 [3, 5632], P(None, 'tp')
- gate_row_norms: float32 [2048], P('fs')
- val_row_norms: float32 [2048], P('fs')
- tap_row_norms: float32 [2, 3], replicated
The draws below stay inside these ranges and needn't reach their ends.
All inputs are finite; a program needn't handle non-finite values.
Results may differ from the reference program's by a relative error of at most 0.017.
Values may be sent and summed in bfloat16 or wider, within the bound.
A program may use at most 128 MiB of HBM per device.

```python
import jax
import jax.numpy as jnp
from jax import lax

D = 2048
FF = 5632
TAPS = 3
SEQ = 1024
TOKENS = 4096
N_TP = 8


def spiked(entries, stream_key, source, target, parts, factor):
    owner, partner = [(jnp.arange(entries.shape[axis_at]) // (entries.shape[axis_at] // parts)).reshape([-1 if axis == axis_at else 1 for axis in range(entries.ndim)]) for axis_at in (source, target)]
    chosen = jax.random.permutation(stream_key, parts)[partner]
    strong = (owner == chosen) | (owner == (partner + parts // 2) % parts)
    return jnp.where(strong, factor * entries, entries)


def shard_levels(stream_key, dims, shards, smallest, top_value):
    def one(dim, parts):
        steps = jax.random.uniform(jax.random.fold_in(jax.random.fold_in(stream_key, 6), dim), (parts,), jnp.float32, smallest / len(shards), top_value / len(shards))
        return jnp.repeat(jnp.exp(steps), dims[dim] // parts).reshape((-1,) + (1,) * (len(dims) - dim - 1))

    factor_of = one(*shards[0])
    for cut in shards[1:]:
        factor_of = factor_of * one(*cut)
    return factor_of


def scatter_about(rng, shape, width, most, split=(), kind=jnp.bfloat16):
    entries = jax.random.normal(rng, shape, jnp.float32) * width
    if len(split) > 0:
        entries = shard_levels(rng, shape, split, -0.22, 0.18) * entries
    return jnp.clip(entries, min=-most, max=most).astype(kind)


def noise_with(own_key, shape, spread, most, pieces, heavy, kind=jnp.bfloat16):
    drawn = spread * jax.random.normal(own_key, shape, jnp.float32)
    if pieces:
        drawn = drawn * shard_levels(own_key, shape, pieces, -0.22, 0.18)
    return jnp.clip(spiked(drawn, jax.random.fold_in(own_key, 3), *heavy), -most, most).astype(kind)


def setup_inputs(seed: int = 0) -> dict:
    arg_keys = jax.random.split(jax.random.key(seed), 9)
    tokens = noise_with(arg_keys[0], (TOKENS, D), 1.0, 6.0, ((0, 32),), (0, 1, 32, 2.75))
    up_gate = scatter_about(arg_keys[1], (TOKENS, FF), 1.5, 8.0, ((0, 4), (1, 8)))
    up_val = scatter_about(arg_keys[2], (TOKENS, FF), 1.0, 6.0, ((0, 4), (1, 8)))
    gate_weight = scatter_about(arg_keys[3], (D, FF), D ** -0.5, 0.125, ((0, 4), (1, 8)))
    val_weight = scatter_about(arg_keys[4], (D, FF), D ** -0.5, 0.125, ((0, 4), (1, 8)))
    gate_taps = scatter_about(arg_keys[5], (TAPS, FF), 0.6, 3.0, ((1, 8),))
    val_taps = scatter_about(arg_keys[6], (TAPS, FF), 0.6, 3.0, ((1, 8),))
    hidden_grad = noise_with(arg_keys[7], (TOKENS, FF), 1.0, 6.0, ((0, 4), (1, 8)), (0, 1, 8, 2.0))
    return {"tokens": tokens, "up_gate": up_gate, "up_val": up_val, "gate_weight": gate_weight, "val_weight": val_weight, "gate_taps": gate_taps, "val_taps": val_taps, "hidden_grad": hidden_grad}


def shifted_sum(padded, kernel, length, backward):
    tap_count = kernel.shape[0]
    result = jnp.zeros((padded.shape[0], length, padded.shape[2]), jnp.float32)
    for tap_index in range(tap_count):
        tap_shift = tap_count - 1 - tap_index if backward else tap_index
        result = result + kernel[tap_index][None, None, :] * padded[:, tap_shift:tap_shift + length]
    return result


def local_grads(up_gate, up_val, hidden_grad, gate_taps, val_taps):
    length = up_gate.shape[1]
    tap_count = gate_taps.shape[0]
    gate_kernel = gate_taps.astype(jnp.float32)
    val_kernel = val_taps.astype(jnp.float32)
    pad_front = ((0, 0), (tap_count - 1, 0), (0, 0))
    pad_back = ((0, 0), (0, tap_count - 1), (0, 0))
    padded_gate = jnp.pad(up_gate.astype(jnp.float32), pad_front)
    padded_val = jnp.pad(up_val.astype(jnp.float32), pad_front)
    conv_gate = shifted_sum(padded_gate, gate_kernel, length, False)
    conv_val = shifted_sum(padded_val, val_kernel, length, False)
    sigmoid_gate = jax.nn.sigmoid(conv_gate)
    grad_hidden = hidden_grad.astype(jnp.float32)
    val_back = grad_hidden * conv_gate * sigmoid_gate
    gate_back = grad_hidden * conv_val * sigmoid_gate * (1.0 + conv_gate * (1.0 - sigmoid_gate))
    up_gate_back = shifted_sum(jnp.pad(gate_back, pad_back), gate_kernel, length, True).astype(jnp.bfloat16)
    up_val_back = shifted_sum(jnp.pad(val_back, pad_back), val_kernel, length, True).astype(jnp.bfloat16)
    tap_gate = jnp.stack([jnp.sum(padded_gate[:, tap_index:tap_index + length] * gate_back, axis=(0, 1))
                          for tap_index in range(tap_count)])
    tap_val = jnp.stack([jnp.sum(padded_val[:, tap_index:tap_index + length] * val_back, axis=(0, 1))
                         for tap_index in range(tap_count)])
    return up_gate_back, up_val_back, tap_gate, tap_val


def reference(tokens, up_gate, up_val, gate_weight, val_weight, gate_taps, val_taps, hidden_grad):
    width_in = tokens.shape[1]
    hidden_units = up_gate.shape[1]
    block_width = hidden_units // N_TP
    seq_count = tokens.shape[0] // SEQ
    gate_float = gate_weight.astype(jnp.float32).reshape(width_in, N_TP, block_width)
    val_float = val_weight.astype(jnp.float32).reshape(width_in, N_TP, block_width)

    def slice_rows(values, row_start):
        return lax.dynamic_slice_in_dim(values, row_start, SEQ, 0)

    def one_sequence(totals, seq_index):
        row_start = (seq_index * SEQ).astype(jnp.int32)
        local_back = local_grads(slice_rows(up_gate, row_start)[None], slice_rows(up_val, row_start)[None],
                                 slice_rows(hidden_grad, row_start)[None], gate_taps, val_taps)
        gate_back = local_back[0][0]
        val_back = local_back[1][0]
        rows_in = slice_rows(tokens, row_start)
        gate_total = totals[0] + jnp.dot(rows_in.T, gate_back, preferred_element_type=jnp.float32)
        val_total = totals[1] + jnp.dot(rows_in.T, val_back, preferred_element_type=jnp.float32)
        tap_gate_total = totals[2] + local_back[2]
        tap_val_total = totals[3] + local_back[3]
        partials = jnp.einsum('sjf,djf->jsd', gate_back.astype(jnp.float32).reshape(SEQ, N_TP, block_width), gate_float)
        partials = partials + jnp.einsum('sjf,djf->jsd', val_back.astype(jnp.float32).reshape(SEQ, N_TP, block_width), val_float)
        rounded = lax.optimization_barrier(partials.astype(jnp.bfloat16))
        input_rows = jnp.sum(rounded.astype(jnp.float32), axis=0).astype(jnp.bfloat16)
        return (gate_total, val_total, tap_gate_total, tap_val_total), input_rows

    tap_count = gate_taps.shape[0]
    init = (jnp.zeros((width_in, hidden_units), jnp.float32), jnp.zeros((width_in, hidden_units), jnp.float32),
            jnp.zeros((tap_count, hidden_units), jnp.float32), jnp.zeros((tap_count, hidden_units), jnp.float32))
    totals, input_rows = lax.scan(one_sequence, init, jnp.arange(seq_count, dtype=jnp.int32))
    gate_grad, val_grad, tap_gate, tap_val = totals
    input_grad = input_rows.reshape(tokens.shape)
    gate_norms = jnp.sum(gate_grad * gate_grad, axis=1)
    val_norms = jnp.sum(val_grad * val_grad, axis=1)
    tap_norms = jnp.stack([jnp.sum(tap_gate * tap_gate, axis=1), jnp.sum(tap_val * tap_val, axis=1)])
    return (input_grad, gate_grad, val_grad, tap_gate, tap_val, gate_norms, val_norms, tap_norms)
```

```python
import jax
import jax.numpy as jnp
from jax import lax
from jax.sharding import PartitionSpec as P

SEQ = 1024
CHUNKS = 4


def shifted_sum(padded, kernel, length, backward):
    tap_count = kernel.shape[0]
    result = jnp.zeros((padded.shape[0], length, padded.shape[2]), jnp.float32)
    for tap_index in range(tap_count):
        tap_shift = tap_count - 1 - tap_index if backward else tap_index
        result = (
            result + kernel[tap_index][None, None, :] * padded[:, tap_shift : tap_shift + length]
        )
    return result


def local_grads(up_gate, up_val, hidden_grad, gate_taps, val_taps):
    length = up_gate.shape[1]
    tap_count = gate_taps.shape[0]
    gate_kernel = gate_taps.astype(jnp.float32)
    val_kernel = val_taps.astype(jnp.float32)
    pad_front = ((0, 0), (tap_count - 1, 0), (0, 0))
    pad_back = ((0, 0), (0, tap_count - 1), (0, 0))
    padded_gate = jnp.pad(up_gate.astype(jnp.float32), pad_front)
    padded_val = jnp.pad(up_val.astype(jnp.float32), pad_front)
    conv_gate = shifted_sum(padded_gate, gate_kernel, length, False)
    conv_val = shifted_sum(padded_val, val_kernel, length, False)
    sigmoid_gate = jax.nn.sigmoid(conv_gate)
    grad_hidden = hidden_grad.astype(jnp.float32)
    val_back = grad_hidden * conv_gate * sigmoid_gate
    gate_back = grad_hidden * conv_val * sigmoid_gate * (1.0 + conv_gate * (1.0 - sigmoid_gate))
    up_gate_back = shifted_sum(jnp.pad(gate_back, pad_back), gate_kernel, length, True).astype(
        jnp.bfloat16
    )
    up_val_back = shifted_sum(jnp.pad(val_back, pad_back), val_kernel, length, True).astype(
        jnp.bfloat16
    )
    tap_gate = jnp.stack(
        [
            jnp.sum(padded_gate[:, tap_index : tap_index + length] * gate_back, axis=(0, 1))
            for tap_index in range(tap_count)
        ]
    )
    tap_val = jnp.stack(
        [
            jnp.sum(padded_val[:, tap_index : tap_index + length] * val_back, axis=(0, 1))
            for tap_index in range(tap_count)
        ]
    )
    return (up_gate_back, up_val_back, tap_gate, tap_val)


def rolled(values, shift, axis):
    size = values.shape[axis]
    if size == 1:
        return values
    return lax.dynamic_slice_in_dim(
        jnp.concatenate((values, values), axis=axis), shift, size, axis=axis
    )


def make_local(fs_size, tp_size):
    rows_b = max(d for d in range(1, fs_size + 1) if fs_size % d == 0 and d * d <= fs_size)
    fb = rows_b
    fa = fs_size // fb
    cores = 2 if tp_size % 2 == 0 else 1
    chips = tp_size // cores

    def from_b(values, dist):
        perm = [
            (a * fb + (b + dist) % fb, a * fb + b) for a in range(fa) for b in range(fb)
        ]
        return lax.ppermute(values, "fs", perm)

    def from_a(values, dist):
        perm = [
            (((a + dist) % fa) * fb + b, a * fb + b) for a in range(fa) for b in range(fb)
        ]
        return lax.ppermute(values, "fs", perm)

    def from_chip(values, dist):
        perm = [
            (((z + dist) % chips) * cores + c, z * cores + c)
            for z in range(chips)
            for c in range(cores)
        ]
        return lax.ppermute(values, "tp", perm)

    def from_core(values):
        perm = [(i ^ 1, i) for i in range(tp_size)]
        return lax.ppermute(values, "tp", perm)

    def sum_fs(values):
        total = values
        for dist in range(1, fb):
            total = total + from_b(values, dist)
        whole = total
        for dist in range(1, fa):
            whole = whole + from_a(total, dist)
        return whole

    def sum_tp(values):
        total = values + from_core(values) if cores == 2 else values
        whole = total
        for dist in range(1, chips):
            whole = whole + from_chip(total, dist)
        return whole

    def local(tokens, up_gate, up_val, gate_weight, val_weight, gate_taps, val_taps, hidden_grad):
        fs_at = lax.axis_index("fs")
        tp_at = lax.axis_index("tp")
        a_at, b_at = fs_at // fb, fs_at % fb
        z_at, c_at = tp_at // cores, tp_at % cores
        rows, hidden = up_gate.shape
        shard, width = tokens.shape
        block = width // fs_size
        wide = fa * block
        seq_count = rows // SEQ

        cols = rolled(rolled(tokens.reshape(shard, fa, fb, block), a_at, 1), b_at, 2)
        mine = [cols[:, :, 0].reshape(shard, wide)]
        for dist in range(1, fb):
            mine.append(from_b(cols[:, :, fb - dist].reshape(shard, wide), dist))
        token_shard = jnp.stack(mine)
        by_chip = jnp.zeros((chips, fb, shard, wide), tokens.dtype)
        by_chip = lax.dynamic_update_slice(by_chip, token_shard[None], (z_at, 0, 0, 0))
        for dist in range(1, chips):
            by_chip = lax.dynamic_update_slice(
                by_chip, from_chip(token_shard, dist)[None], ((z_at + dist) % chips, 0, 0, 0)
            )
        if cores == 2:
            pair = rolled(jnp.stack((by_chip, from_core(by_chip)), axis=1), c_at, 1)
        else:
            pair = by_chip[:, None]
        token_rows = [pair[:, :, d].reshape(rows, wide) for d in range(fb)]

        joined_weight = jnp.concatenate((gate_weight, val_weight), axis=1)
        weights = [joined_weight] + [from_a(joined_weight, d) for d in range(1, fa)]
        weight_rows = jnp.concatenate(weights, axis=0)

        step = hidden // CHUNKS
        backs = [[] for _ in range(fb)]
        tap_parts = []
        for k in range(CHUNKS):
            cut = slice(k * step, (k + 1) * step)

            def as_blocks(values):
                return values[:, cut].reshape(seq_count, SEQ, step)

            gate_back, val_back, tap_gate, tap_val = local_grads(
                as_blocks(up_gate),
                as_blocks(up_val),
                as_blocks(hidden_grad),
                gate_taps[:, cut],
                val_taps[:, cut],
            )
            back = jnp.concatenate(
                (gate_back.reshape(rows, step), val_back.reshape(rows, step)), axis=1
            )
            backs[0].append(back)
            tap_parts.append(jnp.stack((tap_gate, tap_val)))
            for d in range(1, fb):
                backs[d].append(from_b(back, d))

        taps = sum_fs(jnp.concatenate(tap_parts, axis=2))
        tap_norms = sum_tp(jnp.sum(taps * taps, axis=2))

        over_rows = (((0,), (0,)), ((), ()))
        over_hidden = (((1,), (1,)), ((), ()))

        def dot(left, right, dims):
            return lax.dot_general(left, right, dims, preferred_element_type=jnp.float32)

        grads = []
        for k in range(CHUNKS):
            def partial(d_a):
                at = slice(d_a * block, (d_a + 1) * block)
                total = dot(token_rows[0][:, at], backs[0][k], over_rows)
                for d in range(1, fb):
                    total = total + dot(token_rows[d][:, at], backs[d][k], over_rows)
                return total

            total = partial(0)
            for d in range(1, fa):
                total = total + from_a(partial(fa - d).astype(jnp.bfloat16), d).astype(jnp.float32)
            grads.append(total)
        gate_grad = jnp.concatenate([g[:, :step] for g in grads], axis=1)
        val_grad = jnp.concatenate([g[:, step:] for g in grads], axis=1)
        norms = sum_tp(
            jnp.stack(
                (jnp.sum(gate_grad * gate_grad, axis=1), jnp.sum(val_grad * val_grad, axis=1))
            )
        )

        ordered_weight = jnp.concatenate(
            [
                weight_rows[:, part * hidden + k * step : part * hidden + (k + 1) * step]
                for k in range(CHUNKS)
                for part in range(2)
            ],
            axis=1,
        )

        def reduced(d):
            part = dot(jnp.concatenate(backs[d], axis=1), ordered_weight, over_hidden)
            part = part.astype(jnp.bfloat16).reshape(chips, cores, shard, wide)
            if cores == 2:
                part = rolled(part, c_at, 1)
                pair_sum = (
                    part[:, 0].astype(jnp.float32)
                    + from_core(part[:, 1]).astype(jnp.float32)
                ).astype(jnp.bfloat16)
            else:
                pair_sum = part[:, 0]
            pair_sum = rolled(pair_sum, z_at, 0)
            total = pair_sum[0].astype(jnp.float32)
            for dist in range(1, chips):
                total = total + from_chip(pair_sum[chips - dist], dist).astype(jnp.float32)
            return total.astype(jnp.bfloat16)

        placed = [reduced(0)]
        for d in range(1, fb):
            placed.append(None)
        for d in range(1, fb):
            placed[d] = from_b(reduced(fb - d), d)
        whole = jnp.stack([p.reshape(shard, fa, block) for p in placed], axis=2)
        whole = rolled(rolled(whole, (fa - a_at) % fa, 1), (fb - b_at) % fb, 2)
        input_grad = whole.reshape(shard, width)
        return (
            input_grad, gate_grad, val_grad, taps[0], taps[1], norms[0], norms[1], tap_norms,
        )

    return local


def solution(mesh):
    in_specs = (
        P(("fs", "tp"), None),
        P("fs", "tp"),
        P("fs", "tp"),
        P("fs", "tp"),
        P("fs", "tp"),
        P(None, "tp"),
        P(None, "tp"),
        P("fs", "tp"),
    )
    out_specs = (
        P(("fs", "tp"), None),
        P("fs", "tp"),
        P("fs", "tp"),
        P(None, "tp"),
        P(None, "tp"),
        P("fs"),
        P("fs"),
        P(),
    )
    local = make_local(mesh.shape["fs"], mesh.shape["tp"])
    return jax.shard_map(local, mesh=mesh, in_specs=in_specs, out_specs=out_specs, check_vma=False)
```

```python
import functools

import jax
import jax.numpy as jnp
from jax import lax
from jax.experimental import pallas as pl
from jax.experimental.pallas import tpu as pltpu
from jax.sharding import PartitionSpec as P

SEQ = 1024
CHUNKS = 4


def backs_kernel(group, gate_ref, val_ref, grad_ref, gate_tap_ref, val_tap_ref, back_ref, tap_ref):
    step, rows = gate_ref.shape
    taps = gate_tap_ref.shape[1]
    place = lax.broadcasted_iota(jnp.int32, (group, rows), 1) % SEQ

    def one(index, carry):
        at = pl.ds(pl.multiple_of(index * group, group), group)
        gate_kernel = gate_tap_ref[at, :]
        val_kernel = val_tap_ref[at, :]

        def delayed(field, shift):
            if shift == 0:
                return field
            return jnp.where(place >= shift, pltpu.roll(field, shift, 1), 0.0)

        def advanced(field, shift):
            if shift == 0:
                return field
            return jnp.where(place < SEQ - shift, pltpu.roll(field, rows - shift, 1), 0.0)

        def mixed(fields, kernel):
            total = fields[0] * kernel[:, 0:1]
            for i in range(1, taps):
                total = total + fields[i] * kernel[:, i : i + 1]
            return total

        gate_fields = [
            delayed(gate_ref[at, :].astype(jnp.float32), taps - 1 - i) for i in range(taps)
        ]
        val_fields = [delayed(val_ref[at, :].astype(jnp.float32), taps - 1 - i) for i in range(taps)]
        conv_gate = mixed(gate_fields, gate_kernel)
        conv_val = mixed(val_fields, val_kernel)
        sigmoid = jax.nn.sigmoid(conv_gate)
        scaled = grad_ref[at, :].astype(jnp.float32) * sigmoid
        val_back = scaled * conv_gate
        gate_back = scaled * conv_val * (1.0 + conv_gate * (1.0 - sigmoid))
        back_ref[at, :] = mixed(
            [advanced(gate_back, taps - 1 - i) for i in range(taps)], gate_kernel
        ).astype(jnp.bfloat16)
        back_ref[pl.ds(pl.multiple_of(step + index * group, group), group), :] = mixed(
            [advanced(val_back, taps - 1 - i) for i in range(taps)], val_kernel
        ).astype(jnp.bfloat16)
        for i in range(taps):
            tap_ref[at, i : i + 1] = jnp.sum(gate_fields[i] * gate_back, axis=1, keepdims=True)
            tap_ref[at, taps + i : taps + i + 1] = jnp.sum(
                val_fields[i] * val_back, axis=1, keepdims=True
            )
        return carry

    lax.fori_loop(0, step // group, one, 0)


def chunk_backs(k, step, up_gate, up_val, hidden_grad, gate_taps, val_taps):
    rows = up_gate.shape[1]
    taps = gate_taps.shape[1]
    group = 16 if step % 16 == 0 else 8
    field = pl.BlockSpec((step, rows), lambda i: (k, 0))
    tap = pl.BlockSpec((step, taps), lambda i: (k, 0))
    return pl.pallas_call(
        functools.partial(backs_kernel, group),
        grid=(1,),
        in_specs=[field, field, field, tap, tap],
        out_specs=[
            pl.BlockSpec((2 * step, rows), lambda i: (0, 0)),
            pl.BlockSpec((step, 2 * taps), lambda i: (0, 0)),
        ],
        out_shape=[
            jax.ShapeDtypeStruct((2 * step, rows), jnp.bfloat16),
            jax.ShapeDtypeStruct((step, 2 * taps), jnp.float32),
        ],
        cost_estimate=pl.CostEstimate(
            flops=60 * step * rows, bytes_accessed=10 * step * rows, transcendentals=step * rows
        ),
    )(up_gate, up_val, hidden_grad, gate_taps, val_taps)


def make_local(fs_size, tp_size):
    rows_b = max(d for d in range(1, fs_size + 1) if fs_size % d == 0 and d * d <= fs_size)
    fb = rows_b
    fa = fs_size // fb
    cores = 2 if tp_size % 2 == 0 else 1
    chips = tp_size // cores

    def from_b(values, dist):
        perm = [
            (a * fb + (b + dist) % fb, a * fb + b) for a in range(fa) for b in range(fb)
        ]
        return lax.ppermute(values, "fs", perm)

    def from_a(values, dist):
        perm = [
            (((a + dist) % fa) * fb + b, a * fb + b) for a in range(fa) for b in range(fb)
        ]
        return lax.ppermute(values, "fs", perm)

    def from_chip(values, dist):
        perm = [
            (((z + dist) % chips) * cores + c, z * cores + c)
            for z in range(chips)
            for c in range(cores)
        ]
        return lax.ppermute(values, "tp", perm)

    def from_core(values):
        perm = [(i ^ 1, i) for i in range(tp_size)]
        return lax.ppermute(values, "tp", perm)

    def sum_fs(values):
        total = values
        for dist in range(1, fb):
            total = total + from_b(values, dist)
        whole = total
        for dist in range(1, fa):
            whole = whole + from_a(total, dist)
        return whole

    def sum_tp(values):
        total = values + from_core(values) if cores == 2 else values
        whole = total
        for dist in range(1, chips):
            whole = whole + from_chip(total, dist)
        return whole

    def local(tokens, up_gate, up_val, gate_weight, val_weight, gate_taps, val_taps, hidden_grad):
        fs_at = lax.axis_index("fs")
        tp_at = lax.axis_index("tp")
        a_at, b_at = fs_at // fb, fs_at % fb
        z_at, c_at = tp_at // cores, tp_at % cores
        rows, hidden = up_gate.shape
        shard, width = tokens.shape
        block = width // fs_size
        wide = fa * block
        taps = gate_taps.shape[0]
        step = hidden // CHUNKS

        def columns(dist):
            parts = []
            for d in range(fa):
                start = (((a_at + d) % fa) * fb + (b_at + dist) % fb) * block
                parts.append(lax.dynamic_slice(tokens, (0, start), (shard, block)))
            return jnp.concatenate(parts, axis=1)

        mine = [columns(0)]
        for dist in range(1, fb):
            mine.append(from_b(columns(fb - dist), dist))
        token_shard = jnp.stack(mine)

        def chunked(gate, val):
            parts = []
            for k in range(CHUNKS):
                cut = slice(k * step, (k + 1) * step)
                parts += [gate[cut], val[cut]]
            return jnp.concatenate(parts, axis=0)

        weights = [chunked(gate_weight.T, val_weight.T)]
        for d in range(1, fa):
            weights.append(from_a(weights[0], d))

        fields = (up_gate.T, up_val.T, hidden_grad.T)
        tap_fields = (gate_taps.T.astype(jnp.float32), val_taps.T.astype(jnp.float32))
        backs = [[] for _ in range(fb)]
        tap_parts = []
        for k in range(CHUNKS):
            back, tap = chunk_backs(k, step, *fields, *tap_fields)
            backs[0].append(back)
            tap_parts.append(tap)
            for d in range(1, fb):
                backs[d].append(from_b(back, d))

        pieces = [token_shard]
        for dist in range(1, chips):
            pieces.append(from_chip(token_shard, dist))
        pieces = jnp.stack(pieces)
        sides = [pieces] + ([from_core(pieces)] if cores == 2 else [])
        token_rows = []
        for d in range(fb):
            whole = jnp.zeros((tp_size, shard, wide), tokens.dtype)
            for side, held in enumerate(sides):
                core = (c_at + side) % cores
                for dist in range(chips):
                    place = ((z_at + dist) % chips) * cores + core
                    whole = lax.dynamic_update_slice(whole, held[dist, d][None], (place, 0, 0))
            token_rows.append(whole.reshape(rows, wide))

        tap_sums = sum_fs(jnp.concatenate(tap_parts, axis=0).T)
        taps_grad = tap_sums.reshape(2, taps, hidden)
        tap_norms = sum_tp(jnp.sum(taps_grad * taps_grad, axis=2))

        def dot(left, right, dims):
            return lax.dot_general(left, right, dims, preferred_element_type=jnp.float32)

        inner = (((1,), (0,)), ((), ()))
        over_hidden = (((0,), (0,)), ((), ()))

        def reduced(d):
            back = jnp.concatenate(backs[d], axis=0)
            part = jnp.concatenate(
                [dot(back, weight, over_hidden).astype(jnp.bfloat16) for weight in weights], axis=1
            ).reshape(chips, cores, shard, wide)

            def side(core):
                return lax.dynamic_slice_in_dim(part, core, 1, axis=1)[:, 0]

            if cores == 2:
                other = from_core(side(1 - c_at))
                total = side(c_at).astype(jnp.float32) + other.astype(jnp.float32)
                summed = total.astype(jnp.bfloat16)
            else:
                summed = part[:, 0]

            def chip(dist):
                return lax.dynamic_slice_in_dim(summed, (z_at + dist) % chips, 1, axis=0)[0]

            total = chip(0).astype(jnp.float32)
            for dist in range(1, chips):
                total = total + from_chip(chip(chips - dist), dist).astype(jnp.float32)
            return total.astype(jnp.bfloat16)

        own_rows = reduced(0)

        grads = []
        for k in range(CHUNKS):
            def partial(d_a):
                at = slice(d_a * block, (d_a + 1) * block)
                total = dot(backs[0][k], token_rows[0][:, at], inner)
                for d in range(1, fb):
                    total = total + dot(backs[d][k], token_rows[d][:, at], inner)
                return total

            sent = [partial(fa - d).astype(jnp.bfloat16) for d in range(1, fa)]
            total = partial(0)
            for d in range(1, fa):
                total = total + from_a(sent[d - 1], d).astype(jnp.float32)
            grads.append(total)
        gate_grad = jnp.concatenate([g[:step] for g in grads], axis=0)
        val_grad = jnp.concatenate([g[step:] for g in grads], axis=0)
        norms = sum_tp(
            jnp.stack(
                (jnp.sum(gate_grad * gate_grad, axis=0), jnp.sum(val_grad * val_grad, axis=0))
            )
        )

        placed = [own_rows]
        for d in range(1, fb):
            placed.append(from_b(reduced(fb - d), d))
        input_grad = jnp.zeros((shard, width), tokens.dtype)
        for d in range(fb):
            for d_a in range(fa):
                start = (((a_at + d_a) % fa) * fb + (b_at + d) % fb) * block
                input_grad = lax.dynamic_update_slice(
                    input_grad, placed[d][:, d_a * block : (d_a + 1) * block], (0, start)
                )
        return (
            input_grad,
            gate_grad.T,
            val_grad.T,
            taps_grad[0],
            taps_grad[1],
            norms[0],
            norms[1],
            tap_norms,
        )

    return local


def solution(mesh):
    in_specs = (
        P(("fs", "tp"), None),
        P("fs", "tp"),
        P("fs", "tp"),
        P("fs", "tp"),
        P("fs", "tp"),
        P(None, "tp"),
        P(None, "tp"),
        P("fs", "tp"),
    )
    out_specs = (
        P(("fs", "tp"), None),
        P("fs", "tp"),
        P("fs", "tp"),
        P(None, "tp"),
        P(None, "tp"),
        P("fs"),
        P("fs"),
        P(),
    )
    local = make_local(mesh.shape["fs"], mesh.shape["tp"])
    return jax.shard_map(local, mesh=mesh, in_specs=in_specs, out_specs=out_specs, check_vma=False)
```

```python
import functools

import jax
import jax.numpy as jnp
from jax import lax
from jax.experimental import pallas as pl
from jax.experimental.pallas import tpu as pltpu
from jax.sharding import PartitionSpec as P

SEQ = 1024
CHUNKS = 4


def backs_kernel(group, gate_ref, val_ref, grad_ref, kernel_ref, back_ref, tap_ref):
    step, rows = gate_ref.shape
    taps = kernel_ref.shape[1] // 2
    place = lax.broadcasted_iota(jnp.int32, (group, rows), 1) % SEQ

    def one(index, carry):
        at = pl.ds(pl.multiple_of(index * group, group), group)
        gate_kernel = kernel_ref[at, 0:taps]
        val_kernel = kernel_ref[at, taps : 2 * taps]

        def delayed(field, shift):
            if shift == 0:
                return field
            return jnp.where(place >= shift, pltpu.roll(field, shift, 1), 0.0)

        def advanced(field, shift):
            if shift == 0:
                return field
            return jnp.where(place < SEQ - shift, pltpu.roll(field, rows - shift, 1), 0.0)

        def mixed(fields, kernel):
            total = fields[0] * kernel[:, 0:1]
            for i in range(1, taps):
                total = total + fields[i] * kernel[:, i : i + 1]
            return total

        gate_fields = [
            delayed(gate_ref[at, :].astype(jnp.float32), taps - 1 - i) for i in range(taps)
        ]
        val_fields = [delayed(val_ref[at, :].astype(jnp.float32), taps - 1 - i) for i in range(taps)]
        conv_gate = mixed(gate_fields, gate_kernel)
        conv_val = mixed(val_fields, val_kernel)
        sigmoid = jax.nn.sigmoid(conv_gate)
        scaled = grad_ref[at, :].astype(jnp.float32) * sigmoid
        val_back = scaled * conv_gate
        gate_back = scaled * conv_val * (1.0 + conv_gate * (1.0 - sigmoid))
        back_ref[at, :] = mixed(
            [advanced(gate_back, taps - 1 - i) for i in range(taps)], gate_kernel
        ).astype(jnp.bfloat16)
        back_ref[pl.ds(pl.multiple_of(step + index * group, group), group), :] = mixed(
            [advanced(val_back, taps - 1 - i) for i in range(taps)], val_kernel
        ).astype(jnp.bfloat16)
        for i in range(taps):
            tap_ref[at, i : i + 1] = jnp.sum(gate_fields[i] * gate_back, axis=1, keepdims=True)
            tap_ref[at, taps + i : taps + i + 1] = jnp.sum(
                val_fields[i] * val_back, axis=1, keepdims=True
            )
        return carry

    lax.fori_loop(0, step // group, one, 0)


def chunk_backs(k, step, up_gate, up_val, hidden_grad, kernels):
    rows = up_gate.shape[1]
    taps = kernels.shape[1] // 2
    group = 16 if step % 16 == 0 else 8
    field = pl.BlockSpec((step, rows), lambda i: (k, 0))
    tap = pl.BlockSpec((step, 2 * taps), lambda i: (k, 0))
    return pl.pallas_call(
        functools.partial(backs_kernel, group),
        grid=(1,),
        in_specs=[field, field, field, tap],
        out_specs=[
            pl.BlockSpec((2 * step, rows), lambda i: (0, 0)),
            pl.BlockSpec((step, 2 * taps), lambda i: (0, 0)),
        ],
        out_shape=[
            jax.ShapeDtypeStruct((2 * step, rows), jnp.bfloat16),
            jax.ShapeDtypeStruct((step, 2 * taps), jnp.float32),
        ],
        cost_estimate=pl.CostEstimate(
            flops=60 * step * rows, bytes_accessed=10 * step * rows, transcendentals=step * rows
        ),
    )(up_gate, up_val, hidden_grad, kernels)


def rows_kernel(chunks, fa, chips, cores, at_ref, *refs):
    back_refs = refs[:chunks]
    gate_refs = refs[chunks : chunks + fa]
    val_refs = refs[chunks + fa : chunks + 2 * fa]
    out_ref = refs[-1]
    shard = out_ref.shape[2]
    block = gate_refs[0].shape[1]
    step = back_refs[0].shape[0] // 2
    over_hidden = (((0,), (0,)), ((), ()))

    def one(chip, carry):
        span = cores * shard
        at = pl.ds(pl.multiple_of(chip * span, span), span)
        place = lax.rem(chip - at_ref[0] + chips, chips)
        for d in range(fa):
            total = jnp.zeros((span, block), jnp.float32)
            for k in range(chunks):
                back = back_refs[k][:, at]
                cut = slice(k * step, (k + 1) * step)
                weight = jnp.concatenate((gate_refs[d][cut, :], val_refs[d][cut, :]), axis=0)
                total = total + lax.dot_general(
                    back, weight, over_hidden, preferred_element_type=jnp.float32
                )
            total = total.astype(jnp.bfloat16)
            for core in range(cores):
                side = lax.rem(at_ref[1] + core, cores)
                out_ref[side, place, :, d * block : (d + 1) * block] = total[
                    core * shard : (core + 1) * shard
                ]
        return carry

    lax.fori_loop(0, chips, one, 0)


def partial_rows(place, backs, gate_parts, val_parts, chips, cores):
    rows = backs[0].shape[1]
    shard = rows // (chips * cores)
    fa = len(gate_parts)
    hidden, block = gate_parts[0].shape
    vmem = pl.BlockSpec(memory_space=pltpu.VMEM)
    return pl.pallas_call(
        functools.partial(rows_kernel, len(backs), fa, chips, cores),
        in_specs=[pl.BlockSpec(memory_space=pltpu.SMEM)] + [vmem] * (len(backs) + 2 * fa),
        out_specs=vmem,
        out_shape=jax.ShapeDtypeStruct((cores, chips, shard, fa * block), jnp.bfloat16),
        cost_estimate=pl.CostEstimate(
            flops=4 * rows * hidden * fa * block,
            bytes_accessed=4 * hidden * (rows + fa * block) + 2 * rows * fa * block,
            transcendentals=0,
        ),
    )(place, *backs, *gate_parts, *val_parts)


def make_local(fs_size, tp_size):
    rows_b = max(d for d in range(1, fs_size + 1) if fs_size % d == 0 and d * d <= fs_size)
    fb = rows_b
    fa = fs_size // fb
    cores = 2 if tp_size % 2 == 0 else 1
    chips = tp_size // cores

    def from_b(values, dist):
        perm = [
            (a * fb + (b + dist) % fb, a * fb + b) for a in range(fa) for b in range(fb)
        ]
        return lax.ppermute(values, "fs", perm)

    def from_a(values, dist):
        perm = [
            (((a + dist) % fa) * fb + b, a * fb + b) for a in range(fa) for b in range(fb)
        ]
        return lax.ppermute(values, "fs", perm)

    def from_chip(values, dist):
        perm = [
            (((z + dist) % chips) * cores + c, z * cores + c)
            for z in range(chips)
            for c in range(cores)
        ]
        return lax.ppermute(values, "tp", perm)

    def from_core(values):
        perm = [(i ^ 1, i) for i in range(tp_size)]
        return lax.ppermute(values, "tp", perm)

    def sum_fs(values):
        total = values
        for dist in range(1, fb):
            total = total + from_b(values, dist)
        whole = total
        for dist in range(1, fa):
            whole = whole + from_a(total, dist)
        return whole

    def sum_tp(values):
        total = values + from_core(values) if cores == 2 else values
        whole = total
        for dist in range(1, chips):
            whole = whole + from_chip(total, dist)
        return whole

    def local(tokens, up_gate, up_val, gate_weight, val_weight, gate_taps, val_taps, hidden_grad):
        fs_at = lax.axis_index("fs")
        tp_at = lax.axis_index("tp")
        a_at, b_at = fs_at // fb, fs_at % fb
        z_at, c_at = tp_at // cores, tp_at % cores
        rows, hidden = up_gate.shape
        shard, width = tokens.shape
        block = width // fs_size
        wide = fa * block
        taps = gate_taps.shape[0]
        chunks = max(c for c in range(1, CHUNKS + 1) if hidden % (16 * c) == 0)
        step = hidden // chunks

        def columns(dist):
            parts = []
            for d in range(fa):
                start = (((a_at + d) % fa) * fb + (b_at + dist) % fb) * block
                parts.append(lax.dynamic_slice(tokens, (0, start), (shard, block)))
            return jnp.concatenate(parts, axis=1)

        mine = [columns(0)]
        for dist in range(1, fb):
            mine.append(from_b(columns(fb - dist), dist))
        token_shard = jnp.stack(mine)

        gate_parts, val_parts = [gate_weight.T], [val_weight.T]
        for d in range(1, fa):
            gate_parts.append(from_a(gate_parts[0], d))
            val_parts.append(from_a(val_parts[0], d))

        fields = (up_gate.T, up_val.T, hidden_grad.T)
        kernels = jnp.concatenate((gate_taps, val_taps), axis=0).astype(jnp.float32).T
        backs = [[] for _ in range(fb)]
        tap_parts = []
        for k in range(chunks):
            back, tap = chunk_backs(k, step, *fields, kernels)
            backs[0].append(back)
            tap_parts.append(tap)
            for d in range(1, fb):
                backs[d].append(from_b(back, d))

        pieces = [token_shard]
        for dist in range(1, chips):
            pieces.append(from_chip(token_shard, dist))
        pieces = jnp.stack(pieces)
        sides = [pieces] + ([from_core(pieces)] if cores == 2 else [])
        token_rows = []
        for d in range(fb):
            whole = jnp.zeros((tp_size, shard, wide), tokens.dtype)
            for side, held in enumerate(sides):
                core = (c_at + side) % cores
                for dist in range(chips):
                    place = ((z_at + dist) % chips) * cores + core
                    whole = lax.dynamic_update_slice(whole, held[dist, d][None], (place, 0, 0))
            token_rows.append(whole.reshape(rows, wide))

        tap_sums = sum_fs(jnp.concatenate(tap_parts, axis=0).T)
        taps_grad = tap_sums.reshape(2, taps, hidden)
        tap_norms = sum_tp(jnp.sum(taps_grad * taps_grad, axis=2))

        def dot(left, right, dims):
            return lax.dot_general(left, right, dims, preferred_element_type=jnp.float32)

        inner = (((1,), (0,)), ((), ()))

        def reduced(d):
            part = partial_rows(
                jnp.stack((z_at, c_at)).astype(jnp.int32),
                backs[d], gate_parts, val_parts, chips, cores,
            )
            if cores == 2:
                other = from_core(part[1])
                total = part[0].astype(jnp.float32) + other.astype(jnp.float32)
                summed = total.astype(jnp.bfloat16)
            else:
                summed = part[0]

            def chip(dist):
                return summed[dist]

            total = chip(0).astype(jnp.float32)
            for dist in range(1, chips):
                total = total + from_chip(chip(chips - dist), dist).astype(jnp.float32)
            return total.astype(jnp.bfloat16)

        own_rows = reduced(0)

        grads = []
        for k in range(chunks):
            def partial(d_a):
                at = slice(d_a * block, (d_a + 1) * block)
                total = dot(backs[0][k], token_rows[0][:, at], inner)
                for d in range(1, fb):
                    total = total + dot(backs[d][k], token_rows[d][:, at], inner)
                return total

            sent = [partial(fa - d).astype(jnp.bfloat16) for d in range(1, fa)]
            total = partial(0)
            for d in range(1, fa):
                total = total + from_a(sent[d - 1], d).astype(jnp.float32)
            grads.append(total)
        gate_grad = jnp.concatenate([g[:step] for g in grads], axis=0)
        val_grad = jnp.concatenate([g[step:] for g in grads], axis=0)
        norms = sum_tp(
            jnp.stack(
                (jnp.sum(gate_grad * gate_grad, axis=0), jnp.sum(val_grad * val_grad, axis=0))
            ),
        )

        placed = [own_rows]
        for d in range(1, fb):
            placed.append(from_b(reduced(fb - d), d))
        input_grad = jnp.zeros((shard, width), tokens.dtype)
        for d in range(fb):
            for d_a in range(fa):
                start = (((a_at + d_a) % fa) * fb + (b_at + d) % fb) * block
                input_grad = lax.dynamic_update_slice(
                    input_grad, placed[d][:, d_a * block : (d_a + 1) * block], (0, start)
                )
        return (
            input_grad,
            gate_grad.T,
            val_grad.T,
            taps_grad[0],
            taps_grad[1],
            norms[0],
            norms[1],
            tap_norms,
        )

    return local


def solution(mesh):
    in_specs = (
        P(("fs", "tp"), None),
        P("fs", "tp"),
        P("fs", "tp"),
        P("fs", "tp"),
        P("fs", "tp"),
        P(None, "tp"),
        P(None, "tp"),
        P("fs", "tp"),
    )
    out_specs = (
        P(("fs", "tp"), None),
        P("fs", "tp"),
        P("fs", "tp"),
        P(None, "tp"),
        P(None, "tp"),
        P("fs"),
        P("fs"),
        P(),
    )
    local = make_local(mesh.shape["fs"], mesh.shape["tp"])
    return jax.shard_map(local, mesh=mesh, in_specs=in_specs, out_specs=out_specs, check_vma=False)
```
